32 devices in a mesh: row: 8 (over z, y), col: 4 (over x, core).
Axes of the slice: x: 2, y: 2, z: 4, core: 2. Of those that a mesh axis runs over, the one named last changes fastest.
Arguments:
- tokens: bfloat16 [16384, 2048], P(('row', 'col')), may hold values from -6 to 6
- w_mix: bfloat16 [2048, 512], replicated, may hold values from -0.125 to 0.125
- w_gate: bfloat16 [2048, 2048], replicated, may hold values from -0.125 to 0.125
- gate_bias: float32 [2048], replicated, may hold values from -4 to 4
- w_branch: bfloat16 [512, 2048], replicated, may hold values from -0.25 to 0.25
Outputs:
- mixed: bfloat16 [16384, 2048], P(('row', 'col'))
The draws below stay inside these ranges and needn't reach their ends.
All inputs are finite; a program needn't handle non-finite values.
Results may differ from the reference program's by a relative error of at most 0.0083.
Values may be sent and summed in bfloat16 or wider, within the bound.
No kernel may reach another device: no remote copies, remote signals or barrier semaphores. Data moves between devices by JAX's collectives and lax.ppermute only.
A program may use at most 64 MiB of HBM per device.

```python
import jax
import jax.numpy as jnp

D = 2048
FT_GROUPS = 8
GROUP_DIM = 64
FTW = 512
LENGTH = 16384


def block_scale(own_key, dims, split, smallest, largest):
    level, own = 1.0, jax.random.fold_in(own_key, 6)
    for dim, blocks in split:
        heights = jnp.exp(jax.random.uniform(jax.random.fold_in(own, dim), (blocks,), jnp.float32, smallest / len(split), largest / len(split)))
        level = level * jnp.repeat(heights, dims[dim] // blocks).reshape([-1 if axis == dim else 1 for axis in range(len(dims))])
    return level


def scatter_about(own_key, shape, spread, bound, pieces=(), dtype=jnp.bfloat16):
    gain = block_scale(own_key, shape, pieces, -0.22, 0.18) if pieces else 1.0
    entries = jax.random.normal(own_key, shape, jnp.float32) * spread * gain
    return jnp.minimum(jnp.maximum(entries, -bound), bound).astype(dtype)


def setup_inputs(seed: int = 0) -> dict:
    arg_keys = jax.random.split(jax.random.key(seed), 6)
    return {
        "tokens": scatter_about(arg_keys[0], (LENGTH, D), 1.0, 6.0, ((0, 32),)),
        "w_mix": scatter_about(arg_keys[1], (D, FTW), D ** -0.5, 0.125),
        "w_gate": scatter_about(arg_keys[2], (D, D), D ** -0.5, 0.125),
        "gate_bias": scatter_about(arg_keys[3], (D,), 1.0, 4.0, (), jnp.float32),
        "w_branch": scatter_about(arg_keys[4], (FTW, D), FTW ** -0.5, 0.25),
    }


def reference(tokens, w_mix, w_gate, gate_bias, w_branch):
    mixed_in = jnp.dot(tokens, w_mix, preferred_element_type=jnp.float32).astype(jnp.bfloat16)
    grouped = mixed_in.astype(jnp.float32).reshape(LENGTH, FT_GROUPS, GROUP_DIM)
    spectrum = jnp.fft.fft2(grouped, axes=(0, 2), norm="ortho").real
    spectrum = spectrum.reshape(LENGTH, FT_GROUPS * GROUP_DIM).astype(jnp.bfloat16)
    gate = jax.nn.sigmoid(jnp.dot(tokens, w_gate, preferred_element_type=jnp.float32) + gate_bias)
    branch = jnp.dot(spectrum, w_branch, preferred_element_type=jnp.float32)
    return (gate * branch).astype(jnp.bfloat16)
```

```python
import functools
import math

import jax
import jax.numpy as jnp
import numpy as np
from jax import lax
from jax.experimental import pallas as pl
from jax.experimental.pallas import tpu as pltpu
from jax.sharding import PartitionSpec as P

GROUP_DIM = 64
LANES = 128
AXES = ("row", "col")


def wave(left, right, period):
    angle = (np.outer(left, right) % period) * (2.0 * np.pi / period)
    return np.cos(angle), np.sin(angle)


def channel_tables(channels, n_dev):
    slots = channels // n_dev
    pairs = slots // 2
    half = GROUP_DIM // 2
    index = np.arange(GROUP_DIM)
    forward = np.zeros((channels, channels))
    combine = np.zeros((channels, channels))
    for q in range(channels // 2):
        group, d = divmod(q, half)
        base = group * GROUP_DIM
        even = (q // pairs) * slots + q % pairs
        odd = even + pairs
        rows = slice(base, base + GROUP_DIM)
        forward[rows, even] = np.cos(2 * np.pi * (index * d % GROUP_DIM) / GROUP_DIM)
        if d == 0:
            forward[rows, odd] = np.cos(np.pi * index)
            combine[even, base] = 1.0
            combine[odd, base + half] = 1.0
        else:
            forward[rows, odd] = np.sin(2 * np.pi * (index * d % GROUP_DIM) / GROUP_DIM)
            combine[even, base + d] = 1.0
            combine[odd, base + d] = 1.0
            combine[even, base + GROUP_DIM - d] = 1.0
            combine[odd, base + GROUP_DIM - d] = -1.0
    return forward / math.sqrt(GROUP_DIM), combine


def length_tables(n_dev, local_len, slots):
    full_len = n_dev * local_len
    sub = local_len // n_dev
    dev = np.arange(n_dev)
    pos = np.arange(local_len)
    eye = np.eye(slots)
    cos_j, sin_j = wave(dev, dev, n_dev)
    first = np.concatenate(
        [
            np.einsum("cj,st->scjt", table, eye).reshape(slots * n_dev, n_dev * slots)
            for table in (cos_j, -sin_j)
        ]
    )
    cos_t, sin_t = wave(dev, pos, full_len)
    v_n = local_len // LANES
    u_n = sub // v_n
    v, u, big = np.meshgrid(np.arange(v_n), np.arange(u_n), dev, indexing="ij")
    freq = (big * sub + u * v_n + v).reshape(-1)
    cos_m, sin_m = wave(freq, pos, local_len)
    last = np.concatenate([cos_m, sin_m], axis=1) / math.sqrt(full_len)
    f_n = slots // v_n
    source = np.arange(local_len).reshape(v_n, f_n, n_dev).transpose(1, 0, 2).reshape(-1)
    lane_perm = np.zeros((local_len, local_len))
    lane_perm[source, np.arange(local_len)] = 1.0
    source = np.arange(slots * n_dev).reshape(slots, n_dev).T.reshape(-1)
    row_perm = np.zeros((slots * n_dev, slots * n_dev))
    row_perm[np.arange(slots * n_dev), source] = 1.0
    return first, cos_t, sin_t, last, lane_perm, row_perm


def length_kernel(n_dev, slots, flag_ref, x_ref, first_ref, cos_ref, sin_ref, last_ref, lane_ref, row_ref, out_ref, z_ref, a_ref, b_ref):
    rows, lanes = x_ref.shape
    pairs = slots // 2
    f32 = jnp.float32
    y_re = jnp.dot(first_ref[:rows, :], x_ref[...], preferred_element_type=f32)
    y_im = jnp.dot(first_ref[rows:, :], x_ref[...], preferred_element_type=f32)
    cos_t, sin_t = cos_ref[...], sin_ref[...]
    flag = flag_ref[0]
    for slot in range(slots):
        if slot < pairs:
            t_re, t_im = cos_t, -sin_t
        elif slot == pairs:
            t_re = flag * cos_t - (1.0 - flag) * sin_t
            t_im = -flag * sin_t - (1.0 - flag) * cos_t
        else:
            t_re, t_im = -sin_t, -cos_t
        here = slice(slot * n_dev, (slot + 1) * n_dev)
        p_re, p_im = y_re[here, :], y_im[here, :]
        z_ref[here, :lanes] = (p_re * t_re - p_im * t_im).astype(jnp.bfloat16)
        z_ref[here, lanes:] = (p_re * t_im + p_im * t_re).astype(jnp.bfloat16)
    spec = lax.dot_general(last_ref[...], z_ref[...], (((1,), (1,)), ((), ())), preferred_element_type=f32)
    spec = spec.astype(jnp.bfloat16)
    blocks = lanes // LANES
    tall = rows // blocks
    for e in range(blocks):
        for v in range(blocks):
            a_ref[e * tall : (e + 1) * tall, v * LANES : (v + 1) * LANES] = spec[
                v * tall : (v + 1) * tall, e * LANES : (e + 1) * LANES
            ]
    f_n = slots // blocks
    if f_n > 1:
        mixed = jnp.dot(a_ref[...], lane_ref[...], preferred_element_type=f32).astype(jnp.bfloat16)
        wide = lanes // f_n
        for e in range(blocks):
            for f in range(f_n):
                for u in range(f_n):
                    low, high = e * tall + f * n_dev, e * tall + u * n_dev
                    b_ref[low : low + n_dev, u * wide : (u + 1) * wide] = mixed[
                        high : high + n_dev, f * wide : (f + 1) * wide
                    ]
        ordered = b_ref[...]
    else:
        ordered = a_ref[...]
    out_ref[...] = jnp.dot(row_ref[...], ordered, preferred_element_type=f32).astype(jnp.bfloat16)


def shards(tokens, w_mix, w_gate, gate_bias, w_branch):
    n_dev = lax.axis_size(AXES)
    local_len = tokens.shape[0]
    channels = w_mix.shape[1]
    slots = channels // n_dev
    pairs = slots // 2
    bf16, f32 = jnp.bfloat16, jnp.float32
    assert channels == local_len and slots % (local_len // LANES) == 0
    assert (GROUP_DIM // 2) % pairs == 0
    forward, combine = channel_tables(channels, n_dev)
    tables = length_tables(n_dev, local_len, slots)
    first, cos_t, sin_t, last, lane_perm, row_perm = (
        jnp.asarray(t, dtype) for t, dtype in zip(tables, (bf16, f32, f32, bf16, bf16, bf16))
    )
    mixed_in = jnp.dot(tokens, w_mix, preferred_element_type=f32).astype(bf16)
    slotted = lax.dot_general(
        jnp.asarray(forward, bf16), mixed_in, (((0,), (1,)), ((), ())), preferred_element_type=f32
    ).astype(bf16)
    pieces = lax.all_to_all(
        slotted.reshape(n_dev, slots, local_len), AXES, split_axis=0, concat_axis=0, tiled=True
    ).reshape(channels, local_len)
    flag = (lax.axis_index(AXES) * pairs % (GROUP_DIM // 2) == 0).astype(f32).reshape(1)
    vmem = pl.BlockSpec(memory_space=pltpu.VMEM)
    spectra = pl.pallas_call(
        functools.partial(length_kernel, n_dev, slots),
        out_shape=jax.ShapeDtypeStruct((channels, local_len), bf16),
        in_specs=[pl.BlockSpec(memory_space=pltpu.SMEM)] + [vmem] * 7,
        out_specs=vmem,
        scratch_shapes=[
            pltpu.VMEM((channels, 2 * local_len), bf16),
            pltpu.VMEM((channels, local_len), bf16),
            pltpu.VMEM((channels, local_len), bf16),
        ],
        cost_estimate=pl.CostEstimate(
            flops=12 * channels * local_len * local_len, bytes_accessed=6 << 20, transcendentals=0
        ),
        name="length_transform",
    )(flag, pieces, first, cos_t, sin_t, last, lane_perm, row_perm)
    back = lax.all_to_all(
        spectra.reshape(n_dev, slots, local_len), AXES, split_axis=0, concat_axis=0, tiled=True
    ).reshape(channels, local_len)
    gate = jax.nn.sigmoid(jnp.dot(tokens, w_gate, preferred_element_type=f32) + gate_bias)
    spectrum = lax.dot_general(
        back, jnp.asarray(combine, bf16), (((0,), (0,)), ((), ())), preferred_element_type=f32
    ).astype(bf16)
    branch = jnp.dot(spectrum, w_branch, preferred_element_type=f32)
    return (gate * branch).astype(bf16)


def solution(mesh):
    in_specs = (P(AXES, None), P(), P(), P(), P())
    out_specs = P(AXES, None)
    return jax.shard_map(shards, mesh=mesh, in_specs=in_specs, out_specs=out_specs, check_vma=False)
```

```python
import functools
import math

import jax
import jax.numpy as jnp
import numpy as np
from jax import lax
from jax.experimental import pallas as pl
from jax.experimental.pallas import tpu as pltpu
from jax.sharding import PartitionSpec as P

GROUP_DIM = 64
LANES = 128
AXES = ("row", "col")
TILE = 512
NEARLY = 125 << 19
WHOLE = 62 << 20


def wave(left, right, period):
    angle = (np.outer(left, right) % period) * (2.0 * np.pi / period)
    return np.cos(angle), np.sin(angle)


def channel_tables(channels, n_dev):
    slots = channels // n_dev
    pairs = slots // 2
    half = GROUP_DIM // 2
    index = np.arange(GROUP_DIM)
    forward = np.zeros((channels, channels))
    combine = np.zeros((channels, channels))
    for q in range(channels // 2):
        group, d = divmod(q, half)
        base = group * GROUP_DIM
        even = (q // pairs) * slots + q % pairs
        odd = even + pairs
        rows = slice(base, base + GROUP_DIM)
        forward[rows, even] = np.cos(2 * np.pi * (index * d % GROUP_DIM) / GROUP_DIM)
        if d == 0:
            forward[rows, odd] = np.cos(np.pi * index)
            combine[even, base] = 1.0
            combine[odd, base + half] = 1.0
        else:
            forward[rows, odd] = np.sin(2 * np.pi * (index * d % GROUP_DIM) / GROUP_DIM)
            combine[even, base + d] = 1.0
            combine[odd, base + d] = 1.0
            combine[even, base + GROUP_DIM - d] = 1.0
            combine[odd, base + GROUP_DIM - d] = -1.0
    return forward / math.sqrt(GROUP_DIM), combine


def length_tables(n_dev, local_len, slots):
    full_len = n_dev * local_len
    sub = local_len // n_dev
    dev = np.arange(n_dev)
    pos = np.arange(local_len)
    eye = np.eye(slots)
    cos_j, sin_j = wave(dev, dev, n_dev)
    first = np.concatenate(
        [
            np.einsum("cj,st->scjt", table, eye).reshape(slots * n_dev, n_dev * slots)
            for table in (cos_j, -sin_j)
        ]
    )
    cos_t, sin_t = wave(dev, pos, full_len)
    v_n = local_len // LANES
    u_n = sub // v_n
    v, u, big = np.meshgrid(np.arange(v_n), np.arange(u_n), dev, indexing="ij")
    freq = (big * sub + u * v_n + v).reshape(-1)
    cos_m, sin_m = wave(freq, pos, local_len)
    last = np.concatenate([cos_m, sin_m], axis=1) / math.sqrt(full_len)
    f_n = slots // v_n
    source = np.arange(local_len).reshape(v_n, f_n, n_dev).transpose(1, 0, 2).reshape(-1)
    lane_perm = np.zeros((local_len, local_len))
    lane_perm[source, np.arange(local_len)] = 1.0
    source = np.arange(slots * n_dev).reshape(slots, n_dev).T.reshape(-1)
    row_perm = np.zeros((slots * n_dev, slots * n_dev))
    row_perm[np.arange(slots * n_dev), source] = 1.0
    return first, cos_t, sin_t, last, lane_perm, row_perm


def length_kernel(n_dev, slots, x_hbm, first_hbm, cos_hbm, sin_hbm, last_hbm, lane_hbm, row_hbm, out_ref, z_ref, a_ref, b_ref, x_ref, cos_ref, sin_ref, first_ref, last_ref, lane_ref, row_ref, sem):
    rows, lanes = x_ref.shape
    pairs = slots // 2
    f32 = jnp.float32
    upper, lower = pl.ds(0, rows), pl.ds(rows, rows)
    loads = [
        pltpu.make_async_copy(source, target, sem.at[i])
        for i, (source, target) in enumerate(
            (
                (first_hbm.at[upper, :], first_ref.at[upper, :]),
                (first_hbm.at[lower, :], first_ref.at[lower, :]),
                (last_hbm, last_ref),
                (lane_hbm, lane_ref),
                (row_hbm, row_ref),
                (x_hbm, x_ref),
                (cos_hbm, cos_ref),
                (sin_hbm, sin_ref),
            )
        )
    ]
    for i in (5, 0, 1, 6, 7, 2, 3, 4):
        loads[i].start()
    loads[5].wait()
    loads[0].wait()
    y_re = jnp.dot(first_ref[:rows, :], x_ref[...], preferred_element_type=f32)
    loads[1].wait()
    y_im = jnp.dot(first_ref[rows:, :], x_ref[...], preferred_element_type=f32)
    loads[6].wait()
    loads[7].wait()
    cos_t, sin_t = cos_ref[...], sin_ref[...]
    flag = (lax.axis_index(AXES) * pairs % (GROUP_DIM // 2) == 0).astype(f32)
    for slot in range(slots):
        if slot < pairs:
            t_re, t_im = cos_t, -sin_t
        elif slot == pairs:
            t_re = flag * cos_t - (1.0 - flag) * sin_t
            t_im = -flag * sin_t - (1.0 - flag) * cos_t
        else:
            t_re, t_im = -sin_t, -cos_t
        here = slice(slot * n_dev, (slot + 1) * n_dev)
        p_re, p_im = y_re[here, :], y_im[here, :]
        z_ref[here, :lanes] = (p_re * t_re - p_im * t_im).astype(jnp.bfloat16)
        z_ref[here, lanes:] = (p_re * t_im + p_im * t_re).astype(jnp.bfloat16)
    loads[2].wait()
    spec = lax.dot_general(last_ref[...], z_ref[...], (((1,), (1,)), ((), ())), preferred_element_type=f32)
    spec = spec.astype(jnp.bfloat16)
    blocks = lanes // LANES
    tall = rows // blocks
    for e in range(blocks):
        for v in range(blocks):
            a_ref[e * tall : (e + 1) * tall, v * LANES : (v + 1) * LANES] = spec[
                v * tall : (v + 1) * tall, e * LANES : (e + 1) * LANES
            ]
    f_n = slots // blocks
    loads[3].wait()
    if f_n > 1:
        mixed = jnp.dot(a_ref[...], lane_ref[...], preferred_element_type=f32).astype(jnp.bfloat16)
        wide = lanes // f_n
        for e in range(blocks):
            for f in range(f_n):
                for u in range(f_n):
                    low, high = e * tall + f * n_dev, e * tall + u * n_dev
                    b_ref[low : low + n_dev, u * wide : (u + 1) * wide] = mixed[
                        high : high + n_dev, f * wide : (f + 1) * wide
                    ]
        ordered = b_ref[...]
    else:
        ordered = a_ref[...]
    loads[4].wait()
    out_ref[...] = jnp.dot(row_ref[...], ordered, preferred_element_type=f32).astype(jnp.bfloat16)


def project_kernel(steps, tokens_ref, w_ref, forward_ref, out_ref, t_ref, m_ref, sem):
    deep = w_ref.shape[0] // steps
    copies = []
    for k in range(steps):
        part = pl.ds(k * deep, deep)
        pair = (
            pltpu.make_async_copy(tokens_ref.at[:, part], t_ref.at[:, part], sem.at[0, k]),
            pltpu.make_async_copy(w_ref.at[part, :], m_ref.at[part, :], sem.at[1, k]),
        )
        for copy in pair:
            copy.start()
        copies.append(pair)
    total = None
    for k in range(steps):
        for copy in copies[k]:
            copy.wait()
        part = pl.ds(k * deep, deep)
        term = jnp.dot(t_ref[:, part], m_ref[part, :], preferred_element_type=jnp.float32)
        total = term if total is None else total + term
    mixed_in = total.astype(jnp.bfloat16)
    for low in range(0, out_ref.shape[0], LANES):
        out_ref[low : low + LANES, :] = lax.dot_general(
            forward_ref[...],
            mixed_in[:, low : low + LANES],
            (((0,), (1,)), ((), ())),
            preferred_element_type=jnp.float32,
        ).astype(jnp.bfloat16)


def branch_kernel(tiles, back_ref, combine_ref, gate_hbm, w_hbm, out_hbm, g_ref, w_ref, o_ref, spectrum_ref, sem):
    wide = w_ref.shape[1] // tiles
    parts = [pl.ds(i * wide, wide) for i in range(tiles)]
    loads = [
        (
            pltpu.make_async_copy(w_hbm.at[:, part], w_ref.at[:, part], sem.at[0, i]),
            pltpu.make_async_copy(gate_hbm.at[:, part], g_ref.at[:, part], sem.at[1, i]),
        )
        for i, part in enumerate(parts)
    ]
    stores = [pltpu.make_async_copy(o_ref.at[:, part], out_hbm.at[:, part], sem.at[2, i]) for i, part in enumerate(parts)]
    for pair in loads:
        for load in pair:
            load.start()
    for low in range(0, back_ref.shape[0], LANES):
        spectrum_ref[:, low : low + LANES] = lax.dot_general(
            back_ref[low : low + LANES, :],
            combine_ref[...],
            (((0,), (0,)), ((), ())),
            preferred_element_type=jnp.float32,
        ).astype(jnp.bfloat16)
    for part, pair, store in zip(parts, loads, stores):
        for load in pair:
            load.wait()
        branch = jnp.dot(spectrum_ref[...], w_ref[:, part], preferred_element_type=jnp.float32)
        o_ref[:, part] = (g_ref[:, part].astype(jnp.float32) * branch).astype(jnp.bfloat16)
        store.start()
    for store in stores:
        store.wait()


def shards(tokens, w_mix, w_gate, gate_bias, w_branch):
    n_dev = lax.axis_size(AXES)
    local_len = tokens.shape[0]
    channels = w_mix.shape[1]
    slots = channels // n_dev
    pairs = slots // 2
    bf16, f32 = jnp.bfloat16, jnp.float32
    assert channels == local_len and slots % (local_len // LANES) == 0
    assert (GROUP_DIM // 2) % pairs == 0
    forward, combine = channel_tables(channels, n_dev)
    tables = length_tables(n_dev, local_len, slots)
    first, cos_t, sin_t, last, lane_perm, row_perm = (
        jnp.asarray(t, dtype) for t, dtype in zip(tables, (bf16, f32, f32, bf16, bf16, bf16))
    )
    forward, combine = (jnp.asarray(t[:LANES, :LANES], bf16) for t in (forward, combine))
    depth = w_mix.shape[0]
    vmem = pl.BlockSpec(memory_space=pltpu.VMEM)
    hbm = pl.BlockSpec(memory_space=pltpu.HBM)
    steps = max(1, depth // TILE)
    slotted = pl.pallas_call(
        functools.partial(project_kernel, steps),
        out_shape=jax.ShapeDtypeStruct((channels, local_len), bf16),
        in_specs=[hbm, hbm, vmem],
        out_specs=vmem,
        scratch_shapes=[
            pltpu.VMEM(tokens.shape, bf16),
            pltpu.VMEM(w_mix.shape, bf16),
            pltpu.SemaphoreType.DMA((2, steps)),
        ],
        compiler_params=pltpu.CompilerParams(vmem_limit_bytes=WHOLE),
        cost_estimate=pl.CostEstimate(
            flops=2 * local_len * depth * channels, bytes_accessed=2 * depth * (local_len + channels), transcendentals=0
        ),
        name="project",
    )(tokens, w_mix, forward)
    pieces = lax.all_to_all(
        slotted.reshape(n_dev, slots, local_len), AXES, split_axis=0, concat_axis=0, tiled=True
    ).reshape(channels, local_len)
    spectra = pl.pallas_call(
        functools.partial(length_kernel, n_dev, slots),
        out_shape=jax.ShapeDtypeStruct((channels, local_len), bf16),
        in_specs=[hbm] * 7,
        out_specs=vmem,
        scratch_shapes=[
            pltpu.VMEM((channels, 2 * local_len), bf16),
            pltpu.VMEM((channels, local_len), bf16),
            pltpu.VMEM((channels, local_len), bf16),
            pltpu.VMEM((channels, local_len), bf16),
            pltpu.VMEM(cos_t.shape, f32),
            pltpu.VMEM(sin_t.shape, f32),
            pltpu.VMEM(first.shape, bf16),
            pltpu.VMEM(last.shape, bf16),
            pltpu.VMEM(lane_perm.shape, bf16),
            pltpu.VMEM(row_perm.shape, bf16),
            pltpu.SemaphoreType.DMA((8,)),
        ],
        cost_estimate=pl.CostEstimate(
            flops=12 * channels * local_len * local_len, bytes_accessed=6 << 20, transcendentals=0
        ),
        compiler_params=pltpu.CompilerParams(vmem_limit_bytes=NEARLY),
        name="length_transform",
    )(pieces, first, cos_t, sin_t, last, lane_perm, row_perm)
    back = lax.all_to_all(
        spectra.reshape(n_dev, slots, local_len), AXES, split_axis=0, concat_axis=0, tiled=True
    ).reshape(channels, local_len)
    width = w_branch.shape[1]
    tiles = max(1, width // TILE)
    gate = jax.nn.sigmoid(jnp.dot(tokens, w_gate, preferred_element_type=f32) + gate_bias).astype(bf16)
    return pl.pallas_call(
        functools.partial(branch_kernel, tiles),
        out_shape=jax.ShapeDtypeStruct((local_len, width), bf16),
        in_specs=[vmem, vmem, hbm, hbm],
        out_specs=hbm,
        scratch_shapes=[
            pltpu.VMEM((local_len, width), bf16),
            pltpu.VMEM((channels, width), bf16),
            pltpu.VMEM((local_len, width), bf16),
            pltpu.VMEM((local_len, channels), bf16),
            pltpu.SemaphoreType.DMA((3, tiles)),
        ],
        compiler_params=pltpu.CompilerParams(vmem_limit_bytes=WHOLE),
        cost_estimate=pl.CostEstimate(
            flops=2 * local_len * channels * width, bytes_accessed=6 * local_len * width, transcendentals=0
        ),
        name="branch",
    )(back, combine, gate, w_branch)


def solution(mesh):
    in_specs = (P(AXES, None), P(), P(), P(), P())
    out_specs = P(AXES, None)
    return jax.shard_map(shards, mesh=mesh, in_specs=in_specs, out_specs=out_specs, check_vma=False)
```
